32 devices in a mesh: ep: 16 (over z, y, x), tp: 2 (over core).
Axes of the slice: x: 2, y: 2, z: 4, core: 2. Of those that a mesh axis runs over, the one named last changes fastest.
Arguments:
- tokens: bfloat16 [512, 1024], P(('ep', 'tp')), may hold values from -6 to 6
- lengths: int32 [512], P(('ep', 'tp')), may hold values from 1 to 1024
- cache_latent: bfloat16 [512, 1024, 256], P(('ep', 'tp')), may hold values from -700 to 700
- cache_rope: bfloat16 [512, 32, 1024], P(('ep', 'tp')), may hold values from -6 to 6
- attn_gain: bfloat16 [1024], replicated, may hold values from 0.099609375 to 1.8984375
- w_dq: bfloat16 [1024, 512], replicated, may hold values from -0.1875 to 0.1875
- q_gain: bfloat16 [512], replicated, may hold values from 0.099609375 to 1.8984375
- w_q_nope: bfloat16 [512, 1024], replicated, may hold values from -0.25 to 0.25
- w_q_rope: bfloat16 [512, 512], replicated, may hold values from -0.25 to 0.25
- w_dkv: bfloat16 [1024, 256], replicated, may hold values from -0.1875 to 0.1875
- kv_gain: bfloat16 [256], replicated, may hold values from 0.099609375 to 1.8984375
- w_krope: bfloat16 [1024, 32], replicated, may hold values from -0.1875 to 0.1875
- w_uk: bfloat16 [256, 1024], replicated, may hold values from -0.75 to 0.75
- w_uv: bfloat16 [256, 1024], replicated, may hold values from -0.375 to 0.375
- w_o: bfloat16 [1024, 1024], replicated, may hold values from -0.1875 to 0.1875
- post_gain: bfloat16 [1024], replicated, may hold values from 0.099609375 to 1.8984375
- moe_gain: bfloat16 [1024], replicated, may hold values from 0.099609375 to 1.8984375
- routes: int32 [512, 4], P(('ep', 'tp')), may hold values from 0 to 15, all different within a row; in each aligned block of 16 rows (0 to 15, 16 to 31, ...) at most 6 rows name the same one
- route_scores: float32 [512, 4], P(('ep', 'tp')), may hold values from 0.05 to 1
- expert_gate: bfloat16 [16, 1024, 512], P('ep', None, 'tp'), may hold values from -0.1875 to 0.1875
- expert_up: bfloat16 [16, 1024, 512], P('ep', None, 'tp'), may hold values from -0.1875 to 0.1875
- expert_down: bfloat16 [16, 512, 1024], P('ep', 'tp'), may hold values from -0.25 to 0.25
- shared_gate: bfloat16 [1024, 512], replicated, may hold values from -0.1875 to 0.1875
- shared_up: bfloat16 [1024, 512], replicated, may hold values from -0.1875 to 0.1875
- shared_down: bfloat16 [512, 1024], replicated, may hold values from -0.25 to 0.25
- dense_vec: bfloat16 [1024], replicated, may hold values from -0.1875 to 0.1875
- dense_w_gate: bfloat16 [1024, 8192], P(None, ('ep', 'tp')), may hold values from -0.1875 to 0.1875
- dense_w_up: bfloat16 [1024, 8192], P(None, ('ep', 'tp')), may hold values from -0.1875 to 0.1875
- dense_w_down: bfloat16 [8192, 1024], P(('ep', 'tp')), may hold values from -0.125 to 0.125
- out_gain: bfloat16 [1024], replicated, may hold values from 0.099609375 to 1.8984375
Outputs:
- hidden_out: bfloat16 [512, 1024], P(('ep', 'tp'))
- new_latent: bfloat16 [512, 256], P(('ep', 'tp'))
The draws below stay inside these ranges and needn't reach their ends.
Inputs may be any that keep to these rules, and one draw needn't show every extreme that they name: `routes`: each row names 4 different experts. In the 16 rows of one device no expert is named more than 6 times, a bound that some block reaches in some devices' rows.
All inputs are finite; a program needn't handle non-finite values.
Results may differ from the reference program's by a relative error of at most 0.011.
The reference program's roundings to bfloat16 on the way count: a program that leaves them out, or rounds other values in their place, can miss the bound.
Values may be sent and summed in bfloat16 or wider, within the bound.
A program may use at most 128 MiB of HBM per device.

```python
import math
from functools import partial
import jax
import jax.numpy as jnp
import numpy as np
from jax import lax

D = 1024
HEADS = 16
QL = 512
KL = 256
NOPE = 64
ROPE = 32
VDIM = 64
EFF = 512
SFF = 512
DFF = 8192
TOP_K = 4
SEQ_DEV = 16
CACHE_LEN = 1024
EXPERTS = 16
CAP = 6
TOKENS = 512
N_TP = 2


def draw_cache_latent(key, part):
    base = jnp.clip(jax.random.normal(key, (TOKENS, CACHE_LEN, KL), jnp.float32), -6.0, 6.0)
    return base.astype(jnp.bfloat16)


def with_ends(array, own_key, low, largest):
    index_at = [jax.random.randint(jax.random.fold_in(own_key, axis), (), 0, length) for axis, length in enumerate(array.shape)]
    longest = array.shape.index(max(array.shape))
    neighbour = index_at[:longest] + [(index_at[longest] + 1) % array.shape[longest]] + index_at[longest + 1:]
    return array.at[tuple(index_at)].set(low).at[tuple(neighbour)].set(largest)


def raised(drawn, own_key, source, target, shards_of, factor):
    def block_of(position):
        return (jnp.arange(drawn.shape[position]) // (drawn.shape[position] // shards_of)).reshape((-1,) + (1,) * (drawn.ndim - 1 - position))

    near = jax.random.permutation(own_key, shards_of)[block_of(target)]
    far = (block_of(target) + shards_of // 2) % shards_of
    return jnp.where((block_of(source) == near) | (block_of(source) == far), factor * drawn, drawn)


def block_scale(key, extent, cuts, low, largest):
    factor_of, own = 1.0, jax.random.fold_in(key, 6)
    for dim, shards_of in cuts:
        heights = jnp.exp(jax.random.uniform(jax.random.fold_in(own, dim), (shards_of,), jnp.float32, low / len(cuts), largest / len(cuts)))
        factor_of = factor_of * jnp.repeat(heights, extent[dim] // shards_of).reshape([-1 if axis == dim else 1 for axis in range(len(extent))])
    return factor_of


def routed_block(own_key, own, number, rows, number_of, top, bound, skew):
    order = jax.random.permutation(own_key, number_of)
    crowded, ordinary = shares(number_of, rows * top, bound, skew, True), shares(number_of, rows * top, bound, skew, False)
    places = jnp.arange(number_of)

    def named(sizes, offset_by):
        used = int((sizes > 0).sum())
        fixed = max(1, used // 4)
        moved = fixed + (places - fixed + offset_by * (used - fixed)) % max(1, number_of - fixed)
        return jnp.zeros((number_of,), jnp.int32).at[order[jnp.where(places < fixed, places, moved)]].set(jnp.asarray(sizes, jnp.int32))

    sizes = jnp.where(number % 4 == 0, named(crowded, number // 4), named(ordinary, number - number // 4 - 1))
    mixed = jax.random.permutation(jax.random.fold_in(own, 3), number_of)
    donor, receiver = mixed[0:number_of // 2 * 2:2], mixed[1:number_of // 2 * 2:2]
    slack = jnp.minimum(sizes[donor] - 1, bound - sizes[receiver]) // 2
    slack = jnp.where((donor == order[0]) | (receiver == order[0]) | (sizes[receiver] == 0), 0, jnp.maximum(slack, 0))
    moved = jax.random.randint(jax.random.fold_in(own, 4), (number_of // 2,), 0, 1 << 20) % (slack + 1)
    sizes = sizes.at[donor].add(-moved).at[receiver].add(moved)
    labels = jnp.searchsorted(jnp.cumsum(sizes), jnp.arange(rows * top), side="right").astype(jnp.int32)
    table = labels.reshape(top, rows).T
    table = table[jax.random.permutation(jax.random.fold_in(own, 1), rows)]
    offset_by = jax.random.randint(jax.random.fold_in(own, 2), (rows, 1), 0, top)
    return jnp.take_along_axis(table, (jnp.arange(top)[None, :] + offset_by) % top, axis=1)


def shares(count, total, bound, slope, full):
    portions = [(1 << 20) // math.isqrt(standing ** slope) + 1 for standing in range(1, count + 1)]
    largest = bound if full else min(bound, max(-(-total // count), total * portions[0] // sum(portions)))
    least = 1 if total - largest >= count - 1 else 0
    holding, spare = [largest] + [least] * (count - 1), total - largest - least * (count - 1)
    while spare > 0:
        free = [i for i in range(1, count) if holding[i] < largest] or [i for i in range(1, count) if holding[i] < bound]
        mass, budget = sum([portions[i] for i in free]), spare
        for i in free:
            more = min(bound - holding[i], max(1, budget * portions[i] // mass), spare)
            holding[i] = holding[i] + more
            spare = spare - more
    return np.array(holding)


def bell_draw(rng, dims, deviation, reach, shards=(), kind=jnp.bfloat16):
    level = block_scale(rng, dims, shards, -0.22, 0.18) if shards else 1.0
    array = jax.random.normal(rng, dims, jnp.float32) * deviation * level
    return jnp.minimum(jnp.maximum(array, -reach), reach).astype(kind)


def noise_with(rng, dims, deviation, reach, cuts, heavy, kind=jnp.bfloat16):
    array = deviation * jax.random.normal(rng, dims, jnp.float32)
    if cuts:
        array = array * block_scale(rng, dims, cuts, -0.22, 0.18)
    return jnp.clip(raised(array, jax.random.fold_in(rng, 3), *heavy), -reach, reach).astype(kind)


def setup_inputs(seed: int = 0) -> dict:
    key_list = jax.random.split(jax.random.key(seed), 31)
    tokens = bell_draw(key_list[0], (TOKENS, D), 1.0, 6.0, ((0, 32),))
    lengths = with_ends(jax.random.randint(key_list[1], (TOKENS,), 1, CACHE_LEN + 1), jax.random.fold_in(key_list[1], 1), 1, CACHE_LEN).astype(jnp.int32)
    cache_latent = draw_cache_latent(jax.random.fold_in(key_list[30], 71), 0)
    cache_rope = bell_draw(key_list[3], (TOKENS, ROPE, CACHE_LEN), 1.0, 6.0, ((0, 32),))
    attn_gain = jnp.clip(1.0 + 0.18 * jax.random.normal(key_list[4], (D,), jnp.float32), 0.099609375, 1.8984375).astype(jnp.bfloat16)
    w_dq = bell_draw(key_list[5], (D, QL), D ** -0.5, 0.1875)
    q_gain = jnp.clip(1.0 + 0.18 * jax.random.normal(key_list[6], (QL,), jnp.float32), 0.099609375, 1.8984375).astype(jnp.bfloat16)
    w_q_nope = bell_draw(key_list[7], (QL, HEADS * NOPE), QL ** -0.5, 0.25)
    w_q_rope = bell_draw(key_list[8], (QL, HEADS * ROPE), QL ** -0.5, 0.25)
    w_dkv = bell_draw(key_list[9], (D, KL), D ** -0.5, 0.1875)
    kv_gain = jnp.clip(1.0 + 0.18 * jax.random.normal(key_list[10], (KL,), jnp.float32), 0.099609375, 1.8984375).astype(jnp.bfloat16)
    w_krope = bell_draw(key_list[11], (D, ROPE), D ** -0.5, 0.1875)
    w_uk = bell_draw(key_list[12], (KL, HEADS * NOPE), NOPE ** -0.5, 0.75)
    w_uv = bell_draw(key_list[13], (KL, HEADS * VDIM), KL ** -0.5, 0.375)
    w_o = bell_draw(key_list[14], (HEADS * VDIM, D), (HEADS * VDIM) ** -0.5, 0.1875)
    post_gain = jnp.clip(1.0 + 0.18 * jax.random.normal(key_list[15], (D,), jnp.float32), 0.099609375, 1.8984375).astype(jnp.bfloat16)
    moe_gain = jnp.clip(1.0 + 0.18 * jax.random.normal(key_list[16], (D,), jnp.float32), 0.099609375, 1.8984375).astype(jnp.bfloat16)
    routes_keys = jax.random.split(jax.random.fold_in(key_list[17], 1), TOKENS // SEQ_DEV)
    routes_turns = jax.random.permutation(jax.random.fold_in(key_list[17], 3), TOKENS // SEQ_DEV)
    routes = jax.vmap(lambda own, number: routed_block(jax.random.fold_in(key_list[17], 2), own, number, SEQ_DEV, EXPERTS, TOP_K, CAP, 2))(routes_keys, routes_turns).reshape((TOKENS, TOP_K))
    route_scores = jnp.clip(jnp.exp(math.log(1.0) - 2.9957323 * jax.random.uniform(key_list[18], (TOKENS, TOP_K), jnp.float32) ** block_scale(key_list[18], (TOKENS, TOP_K), ((0, 32),), -0.2, 0.2)), 0.05, 1.0)
    expert_gate = bell_draw(key_list[19], (EXPERTS, D, EFF), D ** -0.5, 0.1875, ((0, 16), (2, 2)))
    expert_up = bell_draw(key_list[20], (EXPERTS, D, EFF), D ** -0.5, 0.1875, ((0, 16), (2, 2)))
    expert_down = bell_draw(key_list[21], (EXPERTS, EFF, D), EFF ** -0.5, 0.25, ((0, 16), (1, 2)))
    shared_gate = bell_draw(key_list[22], (D, SFF), D ** -0.5, 0.1875)
    shared_up = bell_draw(key_list[23], (D, SFF), D ** -0.5, 0.1875)
    shared_down = bell_draw(key_list[24], (SFF, D), SFF ** -0.5, 0.25)
    dense_vec = bell_draw(key_list[25], (D,), D ** -0.5, 0.1875)
    dense_w_gate = bell_draw(key_list[26], (D, DFF), D ** -0.5, 0.1875, ((1, 32),))
    dense_w_up = bell_draw(key_list[27], (D, DFF), D ** -0.5, 0.1875, ((1, 32),))
    dense_w_down = noise_with(key_list[28], (DFF, D), DFF ** -0.5, 0.125, ((0, 32),), (0, 1, 32, 2.75))
    out_gain = jnp.clip(1.0 + 0.18 * jax.random.normal(key_list[29], (D,), jnp.float32), 0.099609375, 1.8984375).astype(jnp.bfloat16)
    return dict(tokens=tokens, lengths=lengths, cache_latent=cache_latent, cache_rope=cache_rope, attn_gain=attn_gain, w_dq=w_dq, q_gain=q_gain, w_q_nope=w_q_nope, w_q_rope=w_q_rope, w_dkv=w_dkv, kv_gain=kv_gain, w_krope=w_krope, w_uk=w_uk, w_uv=w_uv, w_o=w_o, post_gain=post_gain, moe_gain=moe_gain, routes=routes, route_scores=route_scores, expert_gate=expert_gate, expert_up=expert_up, expert_down=expert_down, shared_gate=shared_gate, shared_up=shared_up, shared_down=shared_down, dense_vec=dense_vec, dense_w_gate=dense_w_gate, dense_w_up=dense_w_up, dense_w_down=dense_w_down, out_gain=out_gain)


eps = 1e-06
rope_base = 10000.0
routed_scale = 2.5

def rms_scale(value, gain):
    value = value.astype(jnp.float32)
    inverse = lax.rsqrt(lax.optimization_barrier(jnp.mean(value * value, axis=-1, keepdims=True)) + eps)
    return value * inverse * gain.astype(jnp.float32)

def angles(lengths):
    half = ROPE // 2
    freqs = rope_base ** (-jnp.arange(half, dtype=jnp.float32) / half)
    angle = lengths.astype(jnp.float32)[:, None] * freqs[None, :]
    return (jnp.cos(angle), jnp.sin(angle))

def rotate(value, cosine, sine):
    half = value.shape[-1] // 2
    first, second = (value[..., :half], value[..., half:])
    return jnp.concatenate([first * cosine - second * sine, second * cosine + first * sine], axis=-1)

def slot_table(ids, scores, experts, cap):
    rows, top = ids.shape
    norm = scores / lax.optimization_barrier(jnp.sum(scores, axis=1, keepdims=True)) * routed_scale
    flat = ids.reshape(-1)
    onehot = (flat[:, None] == jnp.arange(experts, dtype=jnp.int32)[None, :]).astype(jnp.int32)
    rank = jnp.cumsum(onehot, axis=0) - 1
    hit = onehot[:, :, None] * (rank[:, :, None] == jnp.arange(cap, dtype=jnp.int32)[None, None, :]).astype(jnp.int32)
    owner = jnp.arange(rows * top, dtype=jnp.int32) // top
    token_of = lax.optimization_barrier(jnp.sum(hit * owner[:, None, None], axis=0)).astype(jnp.int32)
    weight_of = lax.optimization_barrier(jnp.sum(hit.astype(norm.dtype) * norm.reshape(-1)[:, None, None], axis=0))
    return (token_of, weight_of)

def attend_block(block, weights):
    tokens, lengths, latent, rope_keys = block
    attn_gain, w_dq, q_gain, w_q_nope, w_q_rope, w_dkv, kv_gain, w_krope, w_uk, w_uv, w_o, post_gain = weights
    f32 = jnp.float32
    bf16 = jnp.bfloat16
    seqs = tokens.shape[0]
    normed = rms_scale(tokens, attn_gain).astype(bf16)
    q_normed = rms_scale(jnp.dot(normed, w_dq, preferred_element_type=f32), q_gain).astype(bf16)
    q_nope = jnp.dot(q_normed, w_q_nope, preferred_element_type=f32).astype(bf16).reshape(seqs, HEADS, NOPE)
    cosine, sine = angles(lengths)
    q_raw = jnp.dot(q_normed, w_q_rope, preferred_element_type=f32).reshape(seqs, HEADS, ROPE)
    q_rot = rotate(q_raw, cosine[:, None, :], sine[:, None, :]).astype(bf16)
    new_latent = rms_scale(jnp.dot(normed, w_dkv, preferred_element_type=f32), kv_gain).astype(bf16)
    new_rope = rotate(jnp.dot(normed, w_krope, preferred_element_type=f32), cosine, sine).astype(bf16)
    query_lat = jnp.einsum('shn,chn->shc', q_nope.astype(f32), w_uk.reshape(KL, HEADS, NOPE).astype(f32)).astype(bf16)
    scale = (NOPE + ROPE) ** (-0.5)
    past = jnp.einsum('shc,slc->shl', query_lat.astype(f32), latent.astype(f32))
    past = (past + jnp.einsum('shr,srl->shl', q_rot.astype(f32), rope_keys.astype(f32))) * scale
    own = jnp.einsum('shc,sc->sh', query_lat.astype(f32), new_latent.astype(f32))
    own = (own + jnp.einsum('shr,sr->sh', q_rot.astype(f32), new_rope.astype(f32))) * scale
    valid = jnp.arange(CACHE_LEN, dtype=jnp.int32)[None, None, :] < lengths[:, None, None]
    top = jnp.maximum(lax.optimization_barrier(jnp.max(jnp.where(valid, past, -1e+30), axis=-1)), own)
    past_weight = jnp.where(valid, jnp.exp(past - top[..., None]), 0.0)
    own_weight = jnp.exp(own - top)
    total = lax.optimization_barrier(jnp.sum(past_weight, axis=-1)) + own_weight
    past_prob = (past_weight / total[..., None]).astype(bf16)
    own_prob = (own_weight / total).astype(bf16)
    mixed = jnp.einsum('shl,slc->shc', past_prob.astype(f32), latent.astype(f32))
    mixed = (mixed + own_prob.astype(f32)[..., None] * new_latent.astype(f32)[:, None, :]).astype(bf16)
    head_out = jnp.einsum('shc,chv->shv', mixed.astype(f32), w_uv.reshape(KL, HEADS, VDIM).astype(f32)).astype(bf16)
    attn_out = jnp.dot(head_out.reshape(seqs, HEADS * VDIM), w_o, preferred_element_type=f32)
    first = (tokens.astype(f32) + rms_scale(attn_out, post_gain)).astype(bf16)
    return (first, new_latent)

def reference(tokens, lengths, cache_latent, cache_rope, attn_gain, w_dq, q_gain, w_q_nope, w_q_rope, w_dkv, kv_gain, w_krope, w_uk, w_uv, w_o, post_gain, moe_gain, routes, route_scores, expert_gate, expert_up, expert_down, shared_gate, shared_up, shared_down, dense_vec, dense_w_gate, dense_w_up, dense_w_down, out_gain):
    f32 = jnp.float32
    bf16 = jnp.bfloat16
    groups = TOKENS // SEQ_DEV
    weights = (attn_gain, w_dq, q_gain, w_q_nope, w_q_rope, w_dkv, kv_gain, w_krope, w_uk, w_uv, w_o, post_gain)
    blocks = (tokens.reshape(groups, SEQ_DEV, D), lengths.reshape(groups, SEQ_DEV), cache_latent.reshape(groups, SEQ_DEV, CACHE_LEN, KL), cache_rope.reshape(groups, SEQ_DEV, ROPE, CACHE_LEN))
    first, new_latent = lax.map(partial(attend_block, weights=weights), blocks)
    first = first.reshape(TOKENS, D)
    new_latent = new_latent.reshape(TOKENS, KL)
    moe_in = rms_scale(first, moe_gain).astype(bf16)
    shared_act = (jax.nn.silu(jnp.dot(moe_in, shared_gate, preferred_element_type=f32)) * jnp.dot(moe_in, shared_up, preferred_element_type=f32)).astype(bf16)
    shared_out = jnp.dot(shared_act, shared_down, preferred_element_type=f32)
    dense_act = (jax.nn.silu(jnp.dot(moe_in, dense_w_gate, preferred_element_type=f32)) * jnp.dot(moe_in, dense_w_up, preferred_element_type=f32)).astype(bf16)
    dense_out = jnp.dot(dense_act, dense_w_down, preferred_element_type=f32)
    gate = jax.nn.sigmoid(jnp.dot(moe_in, dense_vec, preferred_element_type=f32))
    token_all, weight_all = jax.vmap(partial(slot_table, experts=EXPERTS, cap=CAP))(routes.reshape(groups, SEQ_DEV, TOP_K), route_scores.reshape(groups, SEQ_DEV, TOP_K))
    base = (jnp.arange(groups, dtype=jnp.int32) * SEQ_DEV)[:, None]

    def expert_step(routed, expert):
        where_rows = (lax.dynamic_index_in_dim(token_all, expert, 1, keepdims=False) + base).reshape(-1).astype(jnp.int32)
        weight = lax.dynamic_index_in_dim(weight_all, expert, 1, keepdims=False).reshape(-1)
        rows = moe_in[where_rows]
        hidden_gate = jnp.dot(rows, expert_gate[expert], preferred_element_type=f32)
        hidden_up = jnp.dot(rows, expert_up[expert], preferred_element_type=f32)
        act = (jax.nn.silu(hidden_gate) * hidden_up).astype(bf16)
        act_parts = act.astype(f32).reshape(-1, N_TP, EFF // N_TP)
        down_parts = expert_down[expert].astype(f32).reshape(N_TP, EFF // N_TP, D)
        parts = jnp.einsum('rtf,tfd->rtd', act_parts, down_parts).astype(bf16).astype(f32)
        out = lax.optimization_barrier(jnp.sum(parts, axis=1))
        return (routed.at[where_rows].add(out * weight[:, None].astype(f32)), None)
    routed, _ = lax.scan(expert_step, jnp.zeros((TOKENS, D), f32), jnp.arange(EXPERTS, dtype=jnp.int32))
    mixture = routed + shared_out + gate[:, None] * dense_out
    hidden_out = (first.astype(f32) + rms_scale(mixture, out_gain)).astype(bf16)
    return (hidden_out, new_latent)
```

```python
import functools

import jax
import jax.numpy as jnp
from jax import lax
from jax.experimental import pallas as pl
from jax.experimental.pallas import tpu as pltpu
from jax.sharding import PartitionSpec as P

HEADS = 16
NOPE = 64
ROPE = 32
VDIM = 64


eps = 1e-06
rope_base = 10000.0
routed_scale = 2.5


def rms_scale(value, gain):
    value = value.astype(jnp.float32)
    inverse = lax.rsqrt(jnp.mean(value * value, axis=-1, keepdims=True) + eps)
    return value * inverse * gain.astype(jnp.float32)


MESH = pl.DeviceIdType.MESH


def partner(me, k, count):
    other, bit = me, 1
    while bit < count:
        if (k // bit) % 2:
            other = other + bit * (1 - 2 * ((me // bit) % 2))
        bit *= 2
    return other


def bits_of(size):
    return [1 << i for i in range(size.bit_length() - 1)]


def low_bit(m):
    return m & -m


def high_bit(m):
    return 1 << (m.bit_length() - 1)


def layer_kernel(
    count,
    groups,
    *refs,
):
    f32, bf16 = jnp.float32, jnp.bfloat16
    small, hbm, (out_ref, latent_out) = refs[:11], refs[11:30], refs[30:32]
    smalls, bufs = refs[32:43], refs[43:59]
    (query, spun, scores, probs, mixed, rows, route_out, route_in) = refs[59:67]
    (keep, to_sib, from_sib, to_home, from_home) = refs[67:72]
    (small_sem, load_sem, cache_sem, meta_sem, send_sem, row_recv, relay_recv) = refs[72:79]
    sib_recv, home_recv = refs[79:]
    (tokens_ref, lens_ref, routes_ref, scores_ref, attn_gain, q_gain, kv_gain) = smalls[:7]
    post_gain, moe_gain, dense_vec, out_gain = smalls[7:]
    w_dq, w_dkv, w_krope, w_q_nope, w_q_rope, w_uk, latent, rope, w_uv, w_o = bufs[:10]
    s_in, s_down, e_in, e_down, d_in, d_down = bufs[10:]
    seqs, width = tokens_ref.shape
    batches, length, spread = latent.shape
    batch = seqs // batches
    wide = spread // batch
    tall = HEADS * batch
    size = count // groups
    half_width = width // 2
    me = lax.axis_index("ep")
    core = lax.axis_index("tp")
    sibling = (me, 1 - core)

    def peer(k):
        return (partner(me, k, count), core)

    small_loads = [
        pltpu.make_async_copy(src, dst, small_sem.at[i])
        for i, (src, dst) in enumerate(zip(small, smalls))
    ]
    for load in small_loads:
        load.start()

    def wait_small(*ids):
        for i in ids:
            small_loads[i].wait()

    loads = {
        i: pltpu.make_async_copy(hbm[i], bufs[i], load_sem.at[i])
        for i in (0, 1, 2, 3, 4, 5, 8, 9)
    }
    stacked = [
        (hbm[10], s_in.at[0], 10),
        (hbm[11], s_in.at[1], 10),
        (hbm[12], s_down, 11),
        (hbm[13].at[0], e_in.at[0], 12),
        (hbm[14].at[0], e_in.at[1], 12),
        (hbm[17].at[0], e_down, 13),
        (hbm[15], d_in.at[0], 6),
        (hbm[16], d_in.at[1], 6),
        (hbm[18], d_down, 7),
    ]

    def whole(ref, sem):
        return pltpu.make_async_copy(ref, ref, sem)

    def load_cache(b):
        for j in range(batch):
            s = b * batch + j
            dst = latent.at[b, :, pl.ds(j * wide, wide)]
            pltpu.make_async_copy(hbm[6].at[s], dst, cache_sem.at[0, b]).start()
            pltpu.make_async_copy(hbm[7].at[s], rope.at[b, j], cache_sem.at[1, b]).start()

    for i in range(3):
        loads[i].start()

    barrier = pltpu.get_barrier_semaphore()
    pl.semaphore_signal(barrier, inc=1, device_id=sibling, device_id_type=MESH)
    for k in range(1, count):
        other = partner(me, k, count)
        for c in (core, 1 - core):
            pl.semaphore_signal(barrier, inc=1, device_id=(other, c), device_id_type=MESH)

    def mul(a, b):
        return jnp.dot(a, b, preferred_element_type=f32)

    def mul_t(a, b):
        return lax.dot_general(a, b, (((1,), (1,)), ((), ())), preferred_element_type=f32)

    line = lax.broadcasted_iota(jnp.int32, (seqs, 128), 0)
    lane = lax.broadcasted_iota(jnp.int32, (seqs, 128), 1)

    def upright(flat):
        wide_line = lax.broadcasted_iota(jnp.int32, (seqs, seqs), 0)
        wide_lane = lax.broadcasted_iota(jnp.int32, (seqs, seqs), 1)
        return jnp.sum(jnp.where(wide_line == wide_lane, flat, 0.0), axis=1, keepdims=True)

    wait_small(2, 3)
    for i in range(3, 6):
        loads[i].start()
    share = scores_ref[...] / jnp.sum(scores_ref[...], axis=0, keepdims=True) * routed_scale
    routes = routes_ref[...]
    experts = route_out.shape[0]
    expert = lax.broadcasted_iota(jnp.int32, (experts, seqs), 0)
    table = jnp.zeros((experts, seqs), f32)
    for t in range(routes.shape[0]):
        table = table + jnp.where(expert == routes[t : t + 1], share[t : t + 1], 0.0)
    table = jnp.concatenate([table, jnp.zeros((experts, 128 - seqs), f32)], axis=1)
    for e in range(experts):
        route_out[e] = table[e : e + 1]

    wait_small(1)
    lens = jnp.broadcast_to(upright(lens_ref[...][None, :].astype(f32)), (seqs, 128))
    half = ROPE // 2
    freq = jnp.zeros((seqs, 128), f32)
    for i in range(half):
        freq = jnp.where(lane % half == i, float(rope_base ** (-i / half)), freq)
    angle = lens * freq
    cosine = jnp.cos(angle)
    sine = jnp.sin(angle)
    sine = jnp.where(lane % ROPE < half, -sine, sine)

    def spin(raw):
        swapped = jnp.where(
            lane % ROPE < half, pltpu.roll(raw, 128 - half, 1), pltpu.roll(raw, half, 1)
        )
        return (raw * cosine + swapped * sine).astype(bf16).astype(f32)

    wait_small(0, 4)
    tokens = tokens_ref[...].astype(f32)
    normed = rms_scale(tokens, attn_gain[...][None, :]).astype(bf16)
    wait_small(5, 6)
    loads[0].wait()
    load_cache(0)
    q_normed = rms_scale(mul(normed, w_dq[...]), q_gain[...][None, :]).astype(bf16)
    loads[1].wait()
    new_latent = rms_scale(mul(normed, w_dkv[...]), kv_gain[...][None, :]).astype(bf16)
    latent_out[...] = new_latent
    fresh = new_latent.astype(f32)
    loads[2].wait()
    raw = mul_t(normed, w_krope[...])
    new_rope = spin(jnp.concatenate([raw] * (128 // ROPE), axis=1))
    loads[3].wait()
    q_nope = mul(q_normed, w_q_nope[...]).astype(bf16)
    loads[4].wait()
    raw = mul(q_normed, w_q_rope[...])
    per = 128 // ROPE
    for a in range(HEADS // per):
        turned = spin(raw[:, a * 128 : (a + 1) * 128])
        rolled = [turned] + [pltpu.roll(turned, d * ROPE, 1) for d in range(1, per)]
        for j in range(per):
            pick = rolled[0]
            for d in range(1, per):
                pick = jnp.where((line - j) % per == d, rolled[d], pick)
            pick = jnp.where(lane // ROPE == line % per, pick, 0.0)
            h = a * per + j
            for b in range(batches):
                for v in range(batch // per):
                    spun[b, h * batch : (h + 1) * batch, v * 128 : (v + 1) * 128] = jnp.where(
                        (line % batch) // per == v, pick, 0.0
                    )[b * batch : (b + 1) * batch]
    loads[5].wait()
    for i in range(1, batches):
        load_cache(i)
    loads[8].start()
    loads[9].start()
    low = lax.broadcasted_iota(jnp.int32, (seqs, 2 * NOPE), 1) < NOPE
    for pair in range(HEADS // 2):
        at = slice(pair * 2 * NOPE, (pair + 1) * 2 * NOPE)
        both = q_nope[:, at].astype(f32)
        both = jnp.concatenate([jnp.where(low, both, 0.0), jnp.where(low, 0.0, both)], axis=0)
        lat = mul_t(both.astype(bf16), w_uk[:, at]).astype(bf16).astype(f32)
        for i in range(2):
            for b in range(batches):
                h = 2 * pair + i
                query[b, h * batch : (h + 1) * batch, :] = lat[
                    i * seqs + b * batch : i * seqs + (b + 1) * batch
                ]

    pl.semaphore_wait(barrier, 2 * count - 1)

    others = [(c, k) for c in range(2) for k in range(count) if c + k > 0]
    for c, k in others:
        other = partner(me, k, count)
        pltpu.make_async_remote_copy(
            src_ref=route_out.at[other],
            dst_ref=route_in.at[c * count + k - 1],
            send_sem=send_sem.at[0],
            recv_sem=meta_sem.at[0],
            device_id=(other, core if c == 0 else 1 - core),
            device_id_type=MESH,
        ).start()

    scale = (NOPE + ROPE) ** (-0.5)
    pair = 2 * batch
    place = lax.broadcasted_iota(jnp.int32, (pair, length), 1)

    def twice(x):
        return jnp.concatenate([x, x], axis=0)

    def attend(b):
        whole(latent.at[b], cache_sem.at[0, b]).wait()
        whole(rope.at[b], cache_sem.at[1, b]).wait()
        if b == 0:
            for src, dst, i in stacked:
                pltpu.make_async_copy(src, dst, load_sem.at[i]).start()
        mine = query[b]
        row = lax.broadcasted_iota(jnp.int32, (tall, wide), 0) % batch
        spaced = jnp.concatenate(
            [jnp.where(row == j, mine, 0.0).astype(bf16) for j in range(batch)], axis=1
        )
        past = mul_t(latent[b], spaced)
        keys = rope[b].reshape(batch * ROPE, length)
        scores[...] = (past.T + mul(spun[b].astype(bf16), keys)) * scale
        at = slice(b * batch, (b + 1) * batch)
        own_key = twice(fresh[at])
        own_rope = twice(jnp.concatenate([new_rope[at]] * (batch * ROPE // 128), axis=1))
        limit = twice(lens[at])[:, :1].astype(jnp.int32)
        ends = []
        for i in range(HEADS // 2):
            span = slice(i * pair, (i + 1) * pair)
            own = jnp.sum(query[b, span] * own_key, axis=1, keepdims=True)
            own = (own + jnp.sum(spun[b, span] * own_rope, axis=1, keepdims=True)) * scale
            past = scores[span]
            valid = place < limit
            top = jnp.max(jnp.where(valid, past, -1e30), axis=1, keepdims=True)
            top = jnp.maximum(top, own)
            past = jnp.where(valid, jnp.exp(past - top), 0.0)
            own = jnp.exp(own - top)
            total = jnp.sum(past, axis=1, keepdims=True) + own
            probs[span] = past.astype(bf16)
            ends.append((own.astype(bf16).astype(f32), 1.0 / total))
        seen = jnp.zeros((tall, wide), f32)
        for j in range(batch):
            out = mul(probs[...], latent[b, :, j * wide : (j + 1) * wide])
            seen = jnp.where(row == j, out, seen)
        for i, (own, inverse) in enumerate(ends):
            span = slice(i * pair, (i + 1) * pair)
            mixed[b, span] = (seen[span] + own * own_key) * inverse

    for b in range(batches):
        attend(b)

    loads[8].wait()
    parts = []
    for h in range(0, HEADS, 2):
        at = slice(h * VDIM, (h + 2) * VDIM)
        both = jnp.concatenate(
            [mixed[b, (h + i) * batch : (h + i + 1) * batch] for i in range(2) for b in range(batches)],
            axis=0,
        )
        both = mul(both.astype(bf16), w_uv[:, at])
        parts.append(jnp.where(lane < VDIM, both[:seqs], both[seqs:]))
    head_out = jnp.concatenate(parts, axis=1).astype(bf16)
    loads[9].wait()
    wait_small(7, 8)
    first = (tokens + rms_scale(mul(head_out, w_o[...]), post_gain[...][None, :])).astype(bf16)
    moe_in = rms_scale(first, moe_gain[...][None, :]).astype(bf16)
    rows[0, 0] = moe_in

    def row_copy(hop, src, dst, h):
        cut = slice(None) if h is None else pl.ds(h * half_width, half_width)
        return pltpu.make_async_remote_copy(
            src_ref=rows.at[0, src, :, cut],
            dst_ref=rows.at[0, dst, :, cut],
            send_sem=send_sem.at[1],
            recv_sem=row_recv.at[dst],
            device_id=peer(hop),
            device_id_type=MESH,
        )

    def relay_copy(g, m):
        return pltpu.make_async_remote_copy(
            src_ref=rows.at[0, g * size + m],
            dst_ref=rows.at[1, g * size + m],
            send_sem=send_sem.at[2],
            recv_sem=relay_recv.at[g],
            device_id=sibling,
            device_id_type=MESH,
        )

    def sib_copy(g):
        return pltpu.make_async_remote_copy(
            src_ref=to_sib.at[pl.ds(g * size, size)],
            dst_ref=from_sib.at[pl.ds(g * size, size)],
            send_sem=send_sem.at[3],
            recv_sem=sib_recv.at[g],
            device_id=sibling,
            device_id_type=MESH,
        )

    bits = bits_of(size)
    joint = [m for m in range(1, size) if m != low_bit(m)]

    def home_copy(g, m, hop, h):
        cut = slice(None) if h is None else pl.ds(h * half_width, half_width)
        sem = 1 - min(m, 1)
        if m in joint:
            sem = 2 + 2 * joint.index(m) + h
        return pltpu.make_async_remote_copy(
            src_ref=to_home.at[g * size + m, :, cut],
            dst_ref=from_home.at[g * size + m, :, cut],
            send_sem=send_sem.at[4],
            recv_sem=home_recv.at[g, sem],
            device_id=peer(hop),
            device_id_type=MESH,
        )

    def spread_base(g):
        for bit in bits:
            row_copy(bit, g * size, g * size + bit, None).start()
        relay_copy(g, 0).start()

    def arrive_base(g):
        row_copy(1, 0, g * size, None).wait_recv()
        spread_base(g)

    def arrive(g, m):
        k = g * size + m
        row_copy(1, 0, k, None).wait_recv()
        for h in range(2):
            for bit in bits:
                if (bit > high_bit(m)) if h == 0 else (bit < low_bit(m)):
                    row_copy(bit, k, k + bit, h).start()
        relay_copy(g, m).start()

    for g in list(range(groups - 1, 0, -1)):
        row_copy(g * size, 0, g * size, None).start()
    spread_base(0)

    whole(s_in, load_sem.at[10]).wait()
    whole(s_down, load_sem.at[11]).wait()
    hidden = (jax.nn.silu(mul(moe_in, s_in[0])) * mul(moe_in, s_in[1])).astype(bf16)
    shared_out = mul(hidden, s_down[...])

    whole(e_in, load_sem.at[12]).wait()
    whole(e_down, load_sem.at[13]).wait()
    whole(d_in, load_sem.at[6]).wait()
    whole(d_down, load_sem.at[7]).wait()
    whole(route_in, meta_sem.at[0]).wait()
    wait_small(9, 10)
    gate_rows = jnp.broadcast_to(dense_vec[...][None, :], (seqs, width))

    def weight_of(c, k):
        flat = route_out[me] if c + k == 0 else route_in[c * count + k - 1]
        return upright(flat[:, :seqs])

    def compute(g):
        block = rows[:, g * size : (g + 1) * size].reshape(2 * size * seqs, width)
        weights = jnp.concatenate(
            [weight_of(c, g * size + m) for c in range(2) for m in range(size)], axis=0
        )
        gate = jax.nn.sigmoid(mul_t(block, gate_rows)[:, :1])
        act = (jax.nn.silu(mul(block, e_in[0])) * mul(block, e_in[1])).astype(bf16)
        routed = mul(act, e_down[...]).astype(bf16).astype(f32)
        act = (jax.nn.silu(mul(block, d_in[0])) * mul(block, d_in[1])).astype(bf16)
        part = routed * weights + mul(act, d_down[...]) * gate
        part = part.reshape(2, size, seqs, width)
        to_sib[g * size : (g + 1) * size] = part[1].astype(bf16)
        sib_copy(g).start()
        keep[g * size : (g + 1) * size] = part[0]

    def send_home(g, m, h):
        home_copy(g, m, high_bit(m) if h == 0 else low_bit(m), h).start()

    def cut_of(h):
        return slice(h * half_width, (h + 1) * half_width)

    def inward(m, h):
        return [b for b in bits if ((b > high_bit(m)) if h == 0 else (b < low_bit(m)))]

    def home(g):
        sib_copy(g).wait_recv()
        for m in reversed(range(1, size)):
            k = g * size + m
            for h in range(2):
                part = keep[k, :, cut_of(h)] + from_sib[k, :, cut_of(h)].astype(f32)
                if inward(m, h):
                    keep[k, :, cut_of(h)] = part
                else:
                    to_home[k, :, cut_of(h)] = part.astype(bf16)
                    send_home(g, m, h)
        keep[g * size] = keep[g * size] + from_sib[g * size].astype(f32)

    def pass_on(g):
        for m in reversed(range(1, size)):
            k = g * size + m
            for h in range(2):
                if inward(m, h):
                    part = keep[k, :, cut_of(h)]
                    for bit in inward(m, h):
                        home_copy(g, m + bit, 1, h).wait_recv()
                        part = part + from_home[k + bit, :, cut_of(h)].astype(f32)
                    to_home[k, :, cut_of(h)] = part.astype(bf16)
                    send_home(g, m, h)

    def plane_sum(g):
        part = keep[g * size]
        landed = from_home.at[pl.ds(g * size, len(bits))]
        whole(landed, home_recv.at[g, 0]).wait()
        for bit in bits:
            part = part + from_home[g * size + bit].astype(f32)
        return part

    def send_far(g):
        to_home[g * size] = plane_sum(g).astype(bf16)
        home_copy(g, 0, g * size, None).start()

    def wait_relays(g):
        whole(rows.at[1, pl.ds(g * size, size)], relay_recv.at[g]).wait()

    def early(g):
        for m in range(1, size):
            if m not in joint:
                arrive(g, m)

    def late(g):
        for m in joint:
            arrive(g, m)

    def turn(g):
        wait_relays(g)
        compute(g)

    early(0)
    order = list(range(groups - 1, 0, -1))
    for g in order:
        arrive_base(g)
    late(0)
    order = [0] + order
    for g in order[1:]:
        early(g)
        if g == order[1]:
            turn(0)
    for i, g in enumerate(order):
        if i > 0:
            late(g)
            home(order[i - 1])
            if i > 1:
                pass_on(order[i - 2])
            turn(g)
    home(order[-1])
    for i in range(max(0, len(order) - 2), len(order)):
        pass_on(order[i])
    for g in order:
        if g > 0:
            send_far(g)
    total = shared_out + plane_sum(0)
    for g in range(1, groups):
        home_copy(g, 0, 1, None).wait_recv()
        total = total + from_home[g * size].astype(f32)
    inverse = lax.rsqrt(jnp.mean(total * total, axis=-1, keepdims=True) + eps)
    out_ref[...] = (
        first.astype(f32) + total * inverse * out_gain[...][None, :].astype(f32)
    ).astype(bf16)

    whole(route_in, send_sem.at[0]).wait()
    whole(rows.at[0, pl.ds(1, count - 1)], send_sem.at[1]).wait()
    whole(rows.at[0], send_sem.at[2]).wait()
    whole(to_sib, send_sem.at[3]).wait()
    whole(to_home.at[pl.ds(1, count - 1)], send_sem.at[4]).wait()


def shards(
    tokens,
    lengths,
    cache_latent,
    cache_rope,
    attn_gain,
    w_dq,
    q_gain,
    w_q_nope,
    w_q_rope,
    w_dkv,
    kv_gain,
    w_krope,
    w_uk,
    w_uv,
    w_o,
    post_gain,
    moe_gain,
    routes,
    route_scores,
    expert_gate,
    expert_up,
    expert_down,
    shared_gate,
    shared_up,
    shared_down,
    dense_vec,
    dense_w_gate,
    dense_w_up,
    dense_w_down,
    out_gain,
):
    f32, bf16 = jnp.float32, jnp.bfloat16
    count = lax.axis_size("ep")
    groups = min(4, count)
    seqs, width = tokens.shape
    _, length, wide = cache_latent.shape
    batch = 128 // HEADS
    batches = seqs // batch
    small = [tokens, lengths, routes.T, route_scores.T, attn_gain, q_gain, kv_gain]
    small += [post_gain, moe_gain, dense_vec, out_gain]
    big = [w_dq, w_dkv, w_krope.T, w_q_nope, w_q_rope, w_uk, cache_latent, cache_rope, w_uv, w_o]
    big += [shared_gate, shared_up, shared_down, expert_gate, expert_up, dense_w_gate, dense_w_up]
    big += [expert_down, dense_w_down]
    room = [pltpu.VMEM(w.shape, w.dtype) for w in small + big[:10]]
    room[17] = pltpu.VMEM((batches, length, batch * wide), bf16)
    room[18] = pltpu.VMEM((batches, batch) + cache_rope.shape[1:], bf16)
    room += [
        pltpu.VMEM((2,) + shared_gate.shape, bf16),
        pltpu.VMEM(shared_down.shape, bf16),
        pltpu.VMEM((2,) + expert_gate.shape[1:], bf16),
        pltpu.VMEM(expert_down.shape[1:], bf16),
        pltpu.VMEM((2,) + dense_w_gate.shape, bf16),
        pltpu.VMEM(dense_w_down.shape, bf16),
    ]
    vmem = pl.BlockSpec(memory_space=pltpu.VMEM)
    dma = pltpu.SemaphoreType.DMA
    blocks = (count, seqs, width)
    tall = HEADS * batch
    experts = expert_gate.shape[0] * count
    joint = count // groups - (count // groups).bit_length()
    return pl.pallas_call(
        functools.partial(layer_kernel, count, groups),
        out_shape=(pltpu.VMEM((seqs, width), bf16), pltpu.VMEM((seqs, wide), bf16)),
        in_specs=[pl.BlockSpec(memory_space=pltpu.HBM)] * (len(small) + len(big)),
        out_specs=(vmem, vmem),
        scratch_shapes=room
        + [
            pltpu.VMEM((batches, tall, wide), f32),
            pltpu.VMEM((batches, tall, batch * ROPE), f32),
            pltpu.VMEM((tall, length), f32),
            pltpu.VMEM((tall, length), bf16),
            pltpu.VMEM((batches, tall, wide), f32),
            pltpu.VMEM((2,) + blocks, bf16),
            pltpu.VMEM((experts, 1, 128), f32),
            pltpu.VMEM((2 * count - 1, 1, 128), f32),
            pltpu.VMEM(blocks, f32),
            pltpu.VMEM(blocks, bf16),
            pltpu.VMEM(blocks, bf16),
            pltpu.VMEM(blocks, bf16),
            pltpu.VMEM(blocks, bf16),
            dma((len(small),)),
            dma((14,)),
            dma((2, batches)),
            dma((1,)),
            dma((5,)),
            dma((count,)),
            dma((groups,)),
            dma((groups,)),
            dma((groups, 2 + 2 * joint)),
        ],
        compiler_params=pltpu.CompilerParams(collective_id=0, has_side_effects=True),
        name="layer",
    )(*small, *big)


def solution(mesh):
    return jax.shard_map(
        shards,
        mesh=mesh,
        in_specs=(
            P(("ep", "tp"), None),
            P(("ep", "tp")),
            P(("ep", "tp"), None, None),
            P(("ep", "tp"), None, None),
            P(),
            P(),
            P(),
            P(),
            P(),
            P(),
            P(),
            P(),
            P(),
            P(),
            P(),
            P(),
            P(),
            P(("ep", "tp"), None),
            P(("ep", "tp"), None),
            P("ep", None, "tp"),
            P("ep", None, "tp"),
            P("ep", "tp", None),
            P(),
            P(),
            P(),
            P(),
            P(None, ("ep", "tp")),
            P(None, ("ep", "tp")),
            P(("ep", "tp"), None),
            P(),
        ),
        out_specs=(P(("ep", "tp"), None), P(("ep", "tp"), None)),
        check_vma=False,
    )
```

```python
import functools

import jax
import jax.numpy as jnp
from jax import lax
from jax.experimental import pallas as pl
from jax.experimental.pallas import tpu as pltpu
from jax.sharding import PartitionSpec as P

HEADS = 16
NOPE = 64
ROPE = 32
VDIM = 64


eps = 1e-06
rope_base = 10000.0
routed_scale = 2.5


def rms_scale(value, gain):
    value = value.astype(jnp.float32)
    inverse = lax.rsqrt(jnp.mean(value * value, axis=-1, keepdims=True) + eps)
    return value * inverse * gain.astype(jnp.float32)


MESH = pl.DeviceIdType.MESH


def layer_kernel(
    count,
    groups,
    *refs,
):
    f32, bf16 = jnp.float32, jnp.bfloat16
    small, hbm, (out_ref, latent_out) = refs[:11], refs[11:30], refs[30:32]
    smalls, bufs = refs[32:43], refs[43:59]
    (query, spun, scores, probs, mixed, rows, route_out, route_in) = refs[59:67]
    (keep, to_home, from_home) = refs[67:70]
    (small_sem, load_sem, cache_sem, twin_sem, meta_sem, send_sem) = refs[70:76]
    row_recv, near_recv, plane_recv, far_recv = refs[76:]
    (tokens_ref, lens_ref, routes_ref, scores_ref, attn_gain, q_gain, kv_gain) = smalls[:7]
    post_gain, moe_gain, dense_vec, out_gain = smalls[7:]
    w_dq, w_dkv, w_krope, w_q_nope, w_q_rope, w_uk, latent, rope, w_uv, w_o = bufs[:10]
    s_in, s_down, e_in, e_down, d_in, d_down = bufs[10:]
    seqs, width = tokens_ref.shape
    batches, length, spread = latent.shape
    batch = seqs // batches
    wide = spread // batch
    tall = HEADS * batch
    size = count // groups
    me = lax.axis_index("ep")
    core = lax.axis_index("tp")
    flips = {bit: bit * (1 - 2 * ((me // bit) % 2)) for bit in (1 << i for i in range(count.bit_length() - 1))}

    def partner(k):
        other = me
        for bit in flips:
            if k & bit:
                other = other + flips[bit]
        return other

    def peer(k):
        return (partner(k), core)

    small_loads = [
        pltpu.make_async_copy(src, dst, small_sem.at[i])
        for i, (src, dst) in enumerate(zip(small, smalls))
    ]
    for load in small_loads:
        load.start()

    def wait_small(*ids):
        for i in ids:
            small_loads[i].wait()

    loads = {
        i: pltpu.make_async_copy(hbm[i], bufs[i], load_sem.at[i])
        for i in (0, 1, 2, 3, 4, 5, 8, 9)
    }
    stacked = [
        (hbm[10], s_in.at[0], 10),
        (hbm[11], s_in.at[1], 10),
        (hbm[12], s_down, 11),
        (hbm[13].at[0], e_in.at[0, 0], 12),
        (hbm[14].at[0], e_in.at[0, 1], 12),
        (hbm[17].at[0], e_down.at[0], 13),
        (hbm[15], d_in.at[0, 0], 6),
        (hbm[16], d_in.at[0, 1], 6),
        (hbm[18], d_down.at[0], 7),
    ]

    def whole(ref, sem):
        return pltpu.make_async_copy(ref, ref, sem)

    def load_cache(b):
        for j in range(batch):
            s = b * batch + j
            dst = latent.at[b, :, pl.ds(j * wide, wide)]
            pltpu.make_async_copy(hbm[6].at[s], dst, cache_sem.at[0, b]).start()
            pltpu.make_async_copy(hbm[7].at[s], rope.at[b, j], cache_sem.at[1, b]).start()

    for i in range(3):
        loads[i].start()

    barrier = pltpu.get_barrier_semaphore()
    pl.semaphore_signal(barrier, inc=1, device_id=(me, 1 - core), device_id_type=MESH)
    for k in range(1, count):
        pl.semaphore_signal(barrier, inc=1, device_id=peer(k), device_id_type=MESH)

    def mul(a, b):
        return jnp.dot(a, b, preferred_element_type=f32)

    def mul_t(a, b):
        return lax.dot_general(a, b, (((1,), (1,)), ((), ())), preferred_element_type=f32)

    line = lax.broadcasted_iota(jnp.int32, (seqs, 128), 0)
    lane = lax.broadcasted_iota(jnp.int32, (seqs, 128), 1)

    def upright(flat):
        wide_line = lax.broadcasted_iota(jnp.int32, (seqs, seqs), 0)
        wide_lane = lax.broadcasted_iota(jnp.int32, (seqs, seqs), 1)
        return jnp.sum(jnp.where(wide_line == wide_lane, flat, 0.0), axis=1, keepdims=True)

    wait_small(2, 3)
    for i in range(3, 6):
        loads[i].start()
    share = scores_ref[...] / jnp.sum(scores_ref[...], axis=0, keepdims=True) * routed_scale
    routes = routes_ref[...]
    experts = route_out.shape[0]
    expert = lax.broadcasted_iota(jnp.int32, (experts, seqs), 0)
    table = jnp.zeros((experts, seqs), f32)
    for t in range(routes.shape[0]):
        table = table + jnp.where(expert == routes[t : t + 1], share[t : t + 1], 0.0)
    table = jnp.concatenate([table, jnp.zeros((experts, 128 - seqs), f32)], axis=1)
    for e in range(experts):
        route_out[e] = table[e : e + 1]

    wait_small(1)
    lens = jnp.broadcast_to(upright(lens_ref[...][None, :].astype(f32)), (seqs, 128))
    half = ROPE // 2
    freq = jnp.zeros((seqs, 128), f32)
    for i in range(half):
        freq = jnp.where(lane % half == i, float(rope_base ** (-i / half)), freq)
    angle = lens * freq
    cosine = jnp.cos(angle)
    sine = jnp.sin(angle)
    sine = jnp.where(lane % ROPE < half, -sine, sine)

    def spin(raw):
        swapped = jnp.where(
            lane % ROPE < half, pltpu.roll(raw, 128 - half, 1), pltpu.roll(raw, half, 1)
        )
        return (raw * cosine + swapped * sine).astype(bf16).astype(f32)

    wait_small(0, 4)
    tokens = tokens_ref[...].astype(f32)
    normed = rms_scale(tokens, attn_gain[...][None, :]).astype(bf16)
    wait_small(5, 6)
    loads[0].wait()
    load_cache(0)
    q_normed = rms_scale(mul(normed, w_dq[...]), q_gain[...][None, :]).astype(bf16)
    loads[1].wait()
    new_latent = rms_scale(mul(normed, w_dkv[...]), kv_gain[...][None, :]).astype(bf16)
    latent_out[...] = new_latent
    fresh = new_latent.astype(f32)
    loads[2].wait()
    raw = mul_t(normed, w_krope[...])
    new_rope = spin(jnp.concatenate([raw] * (128 // ROPE), axis=1))
    loads[3].wait()
    q_nope = mul(q_normed, w_q_nope[...]).astype(bf16)
    loads[4].wait()
    raw = mul(q_normed, w_q_rope[...])
    per = 128 // ROPE
    for a in range(HEADS // per):
        turned = spin(raw[:, a * 128 : (a + 1) * 128])
        rolled = [turned] + [pltpu.roll(turned, d * ROPE, 1) for d in range(1, per)]
        for j in range(per):
            pick = rolled[0]
            for d in range(1, per):
                pick = jnp.where((line - j) % per == d, rolled[d], pick)
            pick = jnp.where(lane // ROPE == line % per, pick, 0.0)
            h = a * per + j
            for b in range(batches):
                for v in range(batch // per):
                    spun[b, h * batch : (h + 1) * batch, v * 128 : (v + 1) * 128] = jnp.where(
                        (line % batch) // per == v, pick, 0.0
                    )[b * batch : (b + 1) * batch]
    loads[5].wait()
    for i in range(1, batches):
        load_cache(i)
    loads[8].start()
    loads[9].start()
    low = lax.broadcasted_iota(jnp.int32, (seqs, 2 * NOPE), 1) < NOPE
    for pair in range(HEADS // 2):
        at = slice(pair * 2 * NOPE, (pair + 1) * 2 * NOPE)
        both = q_nope[:, at].astype(f32)
        both = jnp.concatenate([jnp.where(low, both, 0.0), jnp.where(low, 0.0, both)], axis=0)
        lat = mul_t(both.astype(bf16), w_uk[:, at]).astype(bf16).astype(f32)
        for i in range(2):
            for b in range(batches):
                h = 2 * pair + i
                query[b, h * batch : (h + 1) * batch, :] = lat[
                    i * seqs + b * batch : i * seqs + (b + 1) * batch
                ]

    pl.semaphore_wait(barrier, count)

    twin = ((e_in, 0), (e_down, 1), (d_in, 2), (d_down, 3))
    into = {13: e_in.at[1, 0], 14: e_in.at[1, 1], 17: e_down.at[1]}
    into.update({15: d_in.at[1, 0], 16: d_in.at[1, 1], 18: d_down.at[1]})
    for i, sem in ((13, 0), (14, 0), (17, 1), (15, 2), (16, 2), (18, 3)):
        pltpu.make_async_remote_copy(
            src_ref=hbm[i].at[0] if len(hbm[i].shape) == 3 else hbm[i],
            dst_ref=into[i],
            send_sem=twin_sem.at[0, sem],
            recv_sem=twin_sem.at[1, sem],
            device_id=(me, 1 - core),
            device_id_type=MESH,
        ).start()

    for k in range(1, count):
        other = partner(k)
        pltpu.make_async_remote_copy(
            src_ref=route_out.at[other],
            dst_ref=route_in.at[k - 1],
            send_sem=send_sem.at[0],
            recv_sem=meta_sem.at[0],
            device_id=(other, core),
            device_id_type=MESH,
        ).start()

    scale = (NOPE + ROPE) ** (-0.5)
    pair = 2 * batch
    place = lax.broadcasted_iota(jnp.int32, (pair, length), 1)

    def twice(x):
        return jnp.concatenate([x, x], axis=0)

    def attend(b):
        whole(latent.at[b], cache_sem.at[0, b]).wait()
        whole(rope.at[b], cache_sem.at[1, b]).wait()
        if b == 0:
            for src, dst, i in stacked:
                pltpu.make_async_copy(src, dst, load_sem.at[i]).start()
        mine = query[b]
        row = lax.broadcasted_iota(jnp.int32, (tall, wide), 0) % batch
        spaced = jnp.concatenate(
            [jnp.where(row == j, mine, 0.0).astype(bf16) for j in range(batch)], axis=1
        )
        keys = rope[b].reshape(batch * ROPE, length)
        turned = spun[b].astype(bf16)
        for r in range(2):
            cut = slice(r * (length // 2), (r + 1) * (length // 2))
            past = mul_t(latent[b, cut], spaced)
            scores[:, cut] = (past.T + mul(turned, keys[:, cut])) * scale
        at = slice(b * batch, (b + 1) * batch)
        own_key = twice(fresh[at])
        own_rope = twice(jnp.concatenate([new_rope[at]] * (batch * ROPE // 128), axis=1))
        limit = twice(lens[at])[:, :1].astype(jnp.int32)
        ends = []
        for i in range(HEADS // 2):
            span = slice(i * pair, (i + 1) * pair)
            own = jnp.sum(query[b, span] * own_key, axis=1, keepdims=True)
            own = (own + jnp.sum(spun[b, span] * own_rope, axis=1, keepdims=True)) * scale
            past = scores[span]
            valid = place < limit
            top = jnp.max(jnp.where(valid, past, -1e30), axis=1, keepdims=True)
            top = jnp.maximum(top, own)
            past = jnp.where(valid, jnp.exp(past - top), 0.0)
            own = jnp.exp(own - top)
            total = jnp.sum(past, axis=1, keepdims=True) + own
            probs[span] = past.astype(bf16)
            ends.append((own.astype(bf16).astype(f32), 1.0 / total))
        seen = jnp.zeros((tall, wide), f32)
        for j in range(batch):
            out = mul(probs[...], latent[b, :, j * wide : (j + 1) * wide])
            seen = jnp.where(row == j, out, seen)
        for i, (own, inverse) in enumerate(ends):
            span = slice(i * pair, (i + 1) * pair)
            mixed[b, span] = (seen[span] + own * own_key) * inverse

    for b in range(batches):
        attend(b)

    loads[8].wait()
    parts = []
    for h in range(0, HEADS, 2):
        at = slice(h * VDIM, (h + 2) * VDIM)
        both = jnp.concatenate(
            [mixed[b, (h + i) * batch : (h + i + 1) * batch] for i in range(2) for b in range(batches)],
            axis=0,
        )
        both = mul(both.astype(bf16), w_uv[:, at])
        parts.append(jnp.where(lane < VDIM, both[:seqs], both[seqs:]))
    head_out = jnp.concatenate(parts, axis=1).astype(bf16)
    loads[9].wait()
    wait_small(7, 8)
    first = (tokens + rms_scale(mul(head_out, w_o[...]), post_gain[...][None, :])).astype(bf16)
    moe_in = rms_scale(first, moe_gain[...][None, :]).astype(bf16)
    rows[0] = moe_in

    def row_copy(hop, src, dst):
        return pltpu.make_async_remote_copy(
            src_ref=rows.at[src],
            dst_ref=rows.at[dst],
            send_sem=send_sem.at[1],
            recv_sem=row_recv.at[dst],
            device_id=peer(hop),
            device_id_type=MESH,
        )

    def home_copy(k, hop, recv_sem):
        return pltpu.make_async_remote_copy(
            src_ref=to_home.at[k],
            dst_ref=from_home.at[k],
            send_sem=send_sem.at[2],
            recv_sem=recv_sem,
            device_id=peer(hop),
            device_id_type=MESH,
        )

    near = [1] if groups > 1 else []
    far = list(range(groups - 1, 1, -1))
    single = [m for m in range(1, size) if m & (m - 1) == 0]
    joint = [m for m in range(1, size) if m & (m - 1)]

    def spread_base(g, ms):
        for m in ms:
            row_copy(m, g * size, g * size + m).start()

    def arrive(k):
        row_copy(1, 0, k).wait_recv()

    for g in far + near:
        row_copy(g * size, 0, g * size).start()
    spread_base(0, single + joint)
    whole(s_in, load_sem.at[10]).wait()
    whole(s_down, load_sem.at[11]).wait()
    hidden = (jax.nn.silu(mul(moe_in, s_in[0])) * mul(moe_in, s_in[1])).astype(bf16)
    shared_out = mul(hidden, s_down[...])

    wait_small(9, 10)
    gate_rows = jnp.broadcast_to(dense_vec[...][None, :], (seqs, width))

    def wait_weights():
        for ref, sem in ((e_in, 12), (e_down, 13), (d_in, 6), (d_down, 7)):
            whole(ref.at[0], load_sem.at[sem]).wait()
        for ref, sem in twin:
            whole(ref.at[1], twin_sem.at[1, sem]).wait()
        whole(route_in, meta_sem.at[0]).wait()

    def weight_of(k):
        flat = route_out[me] if k == 0 else route_in[k - 1]
        return upright(flat[:, :seqs])

    def compute(start, stop):
        lo, hi = start * size, stop * size
        block = rows[lo:hi].reshape((hi - lo) * seqs, width)
        weights = jnp.concatenate([weight_of(k) for k in range(lo, hi)], axis=0)
        gate = jax.nn.sigmoid(mul_t(block, gate_rows)[:, :1])
        pairs = [(ref[c], down[c]) for ref, down in ((e_in, e_down), (d_in, d_down)) for c in range(2)]
        opened = [(mul(block, pair[0]), mul(block, pair[1])) for pair, _ in pairs]
        acts = [(jax.nn.silu(x) * y).astype(bf16) for x, y in opened]
        outs = [mul(x, down) for x, (_, down) in zip(acts, pairs)]
        routed = sum(x.astype(bf16).astype(f32) for x in outs[:2])
        part = routed * weights + (outs[2] + outs[3]) * gate
        keep[lo:hi] = part.reshape(hi - lo, seqs, width)

    def home_near():
        for m in range(size - 1, -1, -1):
            to_home[size + m] = keep[size + m].astype(bf16)
            home_copy(size + m, size, near_recv.at[m]).start()

    def gather_near():
        for m in range(size - 1, -1, -1):
            home_copy(size + m, 1, near_recv.at[m]).wait_recv()
            keep[m] = keep[m] + from_home[size + m].astype(f32)

    def home(g, ms):
        for m in ms:
            to_home[g * size + m] = keep[g * size + m].astype(bf16)
            home_copy(g * size + m, m, plane_recv.at[g]).start()

    def plane_sum(g):
        part = keep[g * size]
        if size > 1:
            whole(from_home.at[pl.ds(g * size + 1, size - 1)], plane_recv.at[g]).wait()
        for m in range(1, size):
            part = part + from_home[g * size + m].astype(f32)
        return part

    def send_far(g):
        to_home[g * size] = plane_sum(g).astype(bf16)
        home_copy(g * size, g * size, far_recv.at[g]).start()

    for m in single:
        arrive(m)
        for g in near:
            row_copy(size, m, size + m).start()
    for g in far:
        arrive(g * size)
        spread_base(g, single)
    for g in far:
        spread_base(g, joint)
    for m in joint:
        arrive(m)
        for g in near:
            row_copy(size, m, size + m).start()
    wait_weights()
    compute(0, 1)
    if near:
        for m in range(size):
            arrive(size + m)
        compute(1, 2)
        home_near()
    if far:
        for k in range(2 * size, count):
            if k % size:
                arrive(k)
        compute(2, groups)
        for g in far:
            home(g, joint + single)
    if near:
        gather_near()
    home(0, joint + single)
    for g in far:
        send_far(g)
    total = shared_out + plane_sum(0)
    for g in far:
        home_copy(g * size, 1, far_recv.at[g]).wait_recv()
        total = total + from_home[g * size].astype(f32)
    inverse = lax.rsqrt(jnp.mean(total * total, axis=-1, keepdims=True) + eps)
    out_ref[...] = (
        first.astype(f32) + total * inverse * out_gain[...][None, :].astype(f32)
    ).astype(bf16)

    for ref, sem in twin:
        whole(ref.at[1], twin_sem.at[0, sem]).wait()
    whole(route_in, send_sem.at[0]).wait()
    whole(rows.at[pl.ds(1, count - 1)], send_sem.at[1]).wait()
    whole(to_home.at[pl.ds(1, count - 1)], send_sem.at[2]).wait()


def shards(
    tokens,
    lengths,
    cache_latent,
    cache_rope,
    attn_gain,
    w_dq,
    q_gain,
    w_q_nope,
    w_q_rope,
    w_dkv,
    kv_gain,
    w_krope,
    w_uk,
    w_uv,
    w_o,
    post_gain,
    moe_gain,
    routes,
    route_scores,
    expert_gate,
    expert_up,
    expert_down,
    shared_gate,
    shared_up,
    shared_down,
    dense_vec,
    dense_w_gate,
    dense_w_up,
    dense_w_down,
    out_gain,
):
    f32, bf16 = jnp.float32, jnp.bfloat16
    count = lax.axis_size("ep")
    groups = min(4, count)
    seqs, width = tokens.shape
    _, length, wide = cache_latent.shape
    batch = 128 // HEADS
    batches = seqs // batch
    small = [tokens, lengths, routes.T, route_scores.T, attn_gain, q_gain, kv_gain]
    small += [post_gain, moe_gain, dense_vec, out_gain]
    big = [w_dq, w_dkv, w_krope.T, w_q_nope, w_q_rope, w_uk, cache_latent, cache_rope, w_uv, w_o]
    big += [shared_gate, shared_up, shared_down, expert_gate, expert_up, dense_w_gate, dense_w_up]
    big += [expert_down, dense_w_down]
    room = [pltpu.VMEM(w.shape, w.dtype) for w in small + big[:10]]
    room[17] = pltpu.VMEM((batches, length, batch * wide), bf16)
    room[18] = pltpu.VMEM((batches, batch) + cache_rope.shape[1:], bf16)
    room += [
        pltpu.VMEM((2,) + shared_gate.shape, bf16),
        pltpu.VMEM(shared_down.shape, bf16),
        pltpu.VMEM((2, 2) + expert_gate.shape[1:], bf16),
        pltpu.VMEM((2,) + expert_down.shape[1:], bf16),
        pltpu.VMEM((2, 2) + dense_w_gate.shape, bf16),
        pltpu.VMEM((2,) + dense_w_down.shape, bf16),
    ]
    vmem = pl.BlockSpec(memory_space=pltpu.VMEM)
    dma = pltpu.SemaphoreType.DMA
    blocks = (count, seqs, width)
    tall = HEADS * batch
    experts = expert_gate.shape[0] * count
    return pl.pallas_call(
        functools.partial(layer_kernel, count, groups),
        out_shape=(pltpu.VMEM((seqs, width), bf16), pltpu.VMEM((seqs, wide), bf16)),
        in_specs=[pl.BlockSpec(memory_space=pltpu.HBM)] * (len(small) + len(big)),
        out_specs=(vmem, vmem),
        scratch_shapes=room
        + [
            pltpu.VMEM((batches, tall, wide), f32),
            pltpu.VMEM((batches, tall, batch * ROPE), f32),
            pltpu.VMEM((tall, length), f32),
            pltpu.VMEM((tall, length), bf16),
            pltpu.VMEM((batches, tall, wide), f32),
            pltpu.VMEM(blocks, bf16),
            pltpu.VMEM((experts, 1, 128), f32),
            pltpu.VMEM((count - 1, 1, 128), f32),
            pltpu.VMEM(blocks, f32),
            pltpu.VMEM(blocks, bf16),
            pltpu.VMEM(blocks, bf16),
            dma((len(small),)),
            dma((14,)),
            dma((2, batches)),
            dma((2, 4)),
            dma((1,)),
            dma((3,)),
            dma((count,)),
            dma((count // groups,)),
            dma((groups,)),
            dma((groups,)),
        ],
        compiler_params=pltpu.CompilerParams(collective_id=0, has_side_effects=True),
        name="layer",
    )(*small, *big)


def solution(mesh):
    return jax.shard_map(
        shards,
        mesh=mesh,
        in_specs=(
            P(("ep", "tp"), None),
            P(("ep", "tp")),
            P(("ep", "tp"), None, None),
            P(("ep", "tp"), None, None),
            P(),
            P(),
            P(),
            P(),
            P(),
            P(),
            P(),
            P(),
            P(),
            P(),
            P(),
            P(),
            P(),
            P(("ep", "tp"), None),
            P(("ep", "tp"), None),
            P("ep", None, "tp"),
            P("ep", None, "tp"),
            P("ep", "tp", None),
            P(),
            P(),
            P(),
            P(),
            P(None, ("ep", "tp")),
            P(None, ("ep", "tp")),
            P(("ep", "tp"), None),
            P(),
        ),
        out_specs=(P(("ep", "tp"), None), P(("ep", "tp"), None)),
        check_vma=False,
    )
```

```python
import functools

import jax
import jax.numpy as jnp
from jax import lax
from jax.experimental import pallas as pl
from jax.experimental.pallas import tpu as pltpu
from jax.sharding import PartitionSpec as P

HEADS = 16
NOPE = 64
ROPE = 32
VDIM = 64


eps = 1e-06
rope_base = 10000.0
routed_scale = 2.5


def rms_scale(value, gain):
    value = value.astype(jnp.float32)
    inverse = lax.rsqrt(jnp.mean(value * value, axis=-1, keepdims=True) + eps)
    return value * inverse * gain.astype(jnp.float32)


MESH = pl.DeviceIdType.MESH


def layer_kernel(
    count,
    groups,
    *refs,
):
    f32, bf16 = jnp.float32, jnp.bfloat16
    small, hbm, (out_ref, latent_out) = refs[:11], refs[11:30], refs[30:32]
    smalls, bufs = refs[32:43], refs[43:59]
    (query, spun, scores, probs, mixed, rows, route_out, route_in) = refs[59:67]
    (keep, to_home, from_home) = refs[67:70]
    (small_sem, load_sem, cache_sem, twin_sem, meta_sem, send_sem) = refs[70:76]
    row_recv, near_recv, plane_recv, far_recv = refs[76:]
    (tokens_ref, lens_ref, routes_ref, scores_ref, attn_gain, q_gain, kv_gain) = smalls[:7]
    post_gain, moe_gain, dense_vec, out_gain = smalls[7:]
    w_dq, w_dkv, w_krope, w_q_nope, w_q_rope, w_uk, latent, rope, w_uv, w_o = bufs[:10]
    s_in, s_down, e_in, e_down, d_in, d_down = bufs[10:]
    seqs, width = tokens_ref.shape
    batches, length, spread = latent.shape
    batch = seqs // batches
    wide = spread // batch
    tall = HEADS * batch
    size = count // groups
    me = lax.axis_index("ep")
    core = lax.axis_index("tp")
    flips = {bit: bit * (1 - 2 * ((me // bit) % 2)) for bit in (1 << i for i in range(count.bit_length() - 1))}

    def partner(k):
        other = me
        for bit in flips:
            if k & bit:
                other = other + flips[bit]
        return other

    def peer(k):
        return (partner(k), core)

    small_loads = [
        pltpu.make_async_copy(src, dst, small_sem.at[i])
        for i, (src, dst) in enumerate(zip(small, smalls))
    ]
    for load in small_loads:
        load.start()

    def wait_small(*ids):
        for i in ids:
            small_loads[i].wait()

    loads = {
        i: pltpu.make_async_copy(hbm[i], bufs[i], load_sem.at[i])
        for i in (0, 1, 2, 3, 4, 5, 8, 9)
    }
    stacked = [
        (hbm[10], s_in.at[0], 10),
        (hbm[11], s_in.at[1], 10),
        (hbm[12], s_down, 11),
        (hbm[13].at[0], e_in.at[0, 0], 12),
        (hbm[14].at[0], e_in.at[0, 1], 12),
        (hbm[17].at[0], e_down.at[0], 13),
        (hbm[15], d_in.at[0, 0], 6),
        (hbm[16], d_in.at[0, 1], 6),
        (hbm[18], d_down.at[0], 7),
    ]

    def whole(ref, sem):
        return pltpu.make_async_copy(ref, ref, sem)

    def load_cache(b):
        for j in range(batch):
            s = b * batch + j
            pltpu.make_async_copy(hbm[7].at[s], rope.at[b, j], cache_sem.at[2, b]).start()
        for r in range(2):
            cut = pl.ds(r * (length // 2), length // 2)
            for j in range(batch):
                src = hbm[6].at[b * batch + j, cut]
                dst = latent.at[b, cut, pl.ds(j * wide, wide)]
                pltpu.make_async_copy(src, dst, cache_sem.at[r, b]).start()

    for i in range(3):
        loads[i].start()

    barrier = pltpu.get_barrier_semaphore()
    pl.semaphore_signal(barrier, inc=1, device_id=(me, 1 - core), device_id_type=MESH)
    for k in range(1, count):
        pl.semaphore_signal(barrier, inc=1, device_id=peer(k), device_id_type=MESH)

    def mul(a, b):
        return jnp.dot(a, b, preferred_element_type=f32)

    def mul_t(a, b):
        return lax.dot_general(a, b, (((1,), (1,)), ((), ())), preferred_element_type=f32)

    line = lax.broadcasted_iota(jnp.int32, (seqs, 128), 0)
    lane = lax.broadcasted_iota(jnp.int32, (seqs, 128), 1)

    def upright(flat):
        wide_line = lax.broadcasted_iota(jnp.int32, (seqs, seqs), 0)
        wide_lane = lax.broadcasted_iota(jnp.int32, (seqs, seqs), 1)
        return jnp.sum(jnp.where(wide_line == wide_lane, flat, 0.0), axis=1, keepdims=True)

    wait_small(2, 3)
    for i in range(3, 6):
        loads[i].start()
    share = scores_ref[...] / jnp.sum(scores_ref[...], axis=0, keepdims=True) * routed_scale
    routes = routes_ref[...]
    experts = route_out.shape[0]
    expert = lax.broadcasted_iota(jnp.int32, (experts, seqs), 0)
    table = jnp.zeros((experts, seqs), f32)
    for t in range(routes.shape[0]):
        table = table + jnp.where(expert == routes[t : t + 1], share[t : t + 1], 0.0)
    table = jnp.concatenate([table, jnp.zeros((experts, 128 - seqs), f32)], axis=1)
    for e in range(experts):
        route_out[e] = table[e : e + 1]

    wait_small(1)
    lens = jnp.broadcast_to(upright(lens_ref[...][None, :].astype(f32)), (seqs, 128))
    half = ROPE // 2
    freq = jnp.zeros((seqs, 128), f32)
    for i in range(half):
        freq = jnp.where(lane % half == i, float(rope_base ** (-i / half)), freq)
    angle = lens * freq
    cosine = jnp.cos(angle)
    sine = jnp.sin(angle)
    sine = jnp.where(lane % ROPE < half, -sine, sine)

    def spin(raw):
        swapped = jnp.where(
            lane % ROPE < half, pltpu.roll(raw, 128 - half, 1), pltpu.roll(raw, half, 1)
        )
        return (raw * cosine + swapped * sine).astype(bf16).astype(f32)

    wait_small(0, 4)
    tokens = tokens_ref[...].astype(f32)
    normed = rms_scale(tokens, attn_gain[...][None, :]).astype(bf16)
    wait_small(5, 6)
    loads[0].wait()
    load_cache(0)
    q_normed = rms_scale(mul(normed, w_dq[...]), q_gain[...][None, :]).astype(bf16)
    for i in range(1, 6):
        loads[i].wait()
    new_latent = rms_scale(mul(normed, w_dkv[...]), kv_gain[...][None, :]).astype(bf16)
    latent_out[...] = new_latent
    fresh = new_latent.astype(f32)
    raw = mul_t(normed, w_krope[...])
    new_rope = spin(jnp.concatenate([raw] * (128 // ROPE), axis=1))
    q_nope = mul(q_normed, w_q_nope[...]).astype(bf16)
    raw = mul(q_normed, w_q_rope[...])
    per = 128 // ROPE
    for a in range(HEADS // per):
        turned = spin(raw[:, a * 128 : (a + 1) * 128])
        rolled = [turned] + [pltpu.roll(turned, d * ROPE, 1) for d in range(1, per)]
        for j in range(per):
            pick = rolled[0]
            for d in range(1, per):
                pick = jnp.where((line - j) % per == d, rolled[d], pick)
            pick = jnp.where(lane // ROPE == line % per, pick, 0.0)
            h = a * per + j
            for b in range(batches):
                for v in range(batch // per):
                    spun[b, h * batch : (h + 1) * batch, v * 128 : (v + 1) * 128] = jnp.where(
                        (line % batch) // per == v, pick, 0.0
                    )[b * batch : (b + 1) * batch]
    low = lax.broadcasted_iota(jnp.int32, (seqs, 2 * NOPE), 1) < NOPE
    for pair in range(HEADS // 2):
        at = slice(pair * 2 * NOPE, (pair + 1) * 2 * NOPE)
        both = q_nope[:, at].astype(f32)
        both = jnp.concatenate([jnp.where(low, both, 0.0), jnp.where(low, 0.0, both)], axis=0)
        lat = mul_t(both.astype(bf16), w_uk[:, at]).astype(bf16).astype(f32)
        for i in range(2):
            for b in range(batches):
                h = 2 * pair + i
                query[b, h * batch : (h + 1) * batch, :] = lat[
                    i * seqs + b * batch : i * seqs + (b + 1) * batch
                ]

    pl.semaphore_wait(barrier, count)

    for i in range(1, batches):
        load_cache(i)
    loads[8].start()
    loads[9].start()
    twin = ((e_in, 0), (e_down, 1), (d_in, 2), (d_down, 3))
    into = {13: e_in.at[1, 0], 14: e_in.at[1, 1], 17: e_down.at[1]}
    into.update({15: d_in.at[1, 0], 16: d_in.at[1, 1], 18: d_down.at[1]})
    for i, sem in ((13, 0), (14, 0), (17, 1), (15, 2), (16, 2), (18, 3)):
        pltpu.make_async_remote_copy(
            src_ref=hbm[i].at[0] if len(hbm[i].shape) == 3 else hbm[i],
            dst_ref=into[i],
            send_sem=twin_sem.at[0, sem],
            recv_sem=twin_sem.at[1, sem],
            device_id=(me, 1 - core),
            device_id_type=MESH,
        ).start()

    for k in range(1, count):
        other = partner(k)
        pltpu.make_async_remote_copy(
            src_ref=route_out.at[other],
            dst_ref=route_in.at[k - 1],
            send_sem=send_sem.at[0],
            recv_sem=meta_sem.at[0],
            device_id=(other, core),
            device_id_type=MESH,
        ).start()

    scale = (NOPE + ROPE) ** (-0.5)
    pair = 2 * batch
    place = lax.broadcasted_iota(jnp.int32, (pair, length), 1)

    def twice(x):
        return jnp.concatenate([x, x], axis=0)

    def attend(b):
        if b > 0:
            for r in range(2):
                half_cut = slice(r * (length // 2), (r + 1) * (length // 2))
                whole(latent.at[b, half_cut], cache_sem.at[r, b]).wait()
            whole(rope.at[b], cache_sem.at[2, b]).wait()
        mine = query[b]
        row = lax.broadcasted_iota(jnp.int32, (tall, wide), 0) % batch
        spaced = jnp.concatenate(
            [jnp.where(row == j, mine, 0.0).astype(bf16) for j in range(batch)], axis=1
        )
        turned = spun[b].astype(bf16)
        for r in range(2):
            half_cut = slice(r * (length // 2), (r + 1) * (length // 2))
            if b == 0:
                whole(latent.at[b, half_cut], cache_sem.at[r, b]).wait()
            if b == 0 and r == 0:
                whole(rope.at[b], cache_sem.at[2, b]).wait()
            parts = 2 if b == 0 else 1
            for i in range(parts):
                long = length // 2 // parts
                cut = slice((parts * r + i) * long, (parts * r + i + 1) * long)
                past = mul_t(latent[b, cut], spaced)
                turning = mul(turned, rope[b].reshape(batch * ROPE, length)[:, cut])
                scores[:, cut] = (past.T + turning) * scale
        if b == 0:
            for src, dst, i in stacked:
                pltpu.make_async_copy(src, dst, load_sem.at[i]).start()
        at = slice(b * batch, (b + 1) * batch)
        own_key = twice(fresh[at])
        own_rope = twice(jnp.concatenate([new_rope[at]] * (batch * ROPE // 128), axis=1))
        limit = twice(lens[at])[:, :1].astype(jnp.int32)
        ends = []
        for i in range(HEADS // 2):
            span = slice(i * pair, (i + 1) * pair)
            own = jnp.sum(query[b, span] * own_key, axis=1, keepdims=True)
            own = (own + jnp.sum(spun[b, span] * own_rope, axis=1, keepdims=True)) * scale
            past = scores[span]
            valid = place < limit
            top = jnp.max(jnp.where(valid, past, -1e30), axis=1, keepdims=True)
            top = jnp.maximum(top, own)
            past = jnp.where(valid, jnp.exp(past - top), 0.0)
            own = jnp.exp(own - top)
            total = jnp.sum(past, axis=1, keepdims=True) + own
            probs[span] = past.astype(bf16)
            ends.append((own.astype(bf16).astype(f32), 1.0 / total))
        seen = jnp.zeros((tall, wide), f32)
        for j in range(batch):
            out = mul(probs[...], latent[b, :, j * wide : (j + 1) * wide])
            seen = jnp.where(row == j, out, seen)
        for i, (own, inverse) in enumerate(ends):
            span = slice(i * pair, (i + 1) * pair)
            mixed[b, span] = (seen[span] + own * own_key) * inverse

    for b in range(batches):
        attend(b)

    loads[8].wait()
    parts = []
    for h in range(0, HEADS, 2):
        at = slice(h * VDIM, (h + 2) * VDIM)
        both = jnp.concatenate(
            [mixed[b, (h + i) * batch : (h + i + 1) * batch] for i in range(2) for b in range(batches)],
            axis=0,
        )
        both = mul(both.astype(bf16), w_uv[:, at])
        parts.append(jnp.where(lane < VDIM, both[:seqs], both[seqs:]))
    head_out = jnp.concatenate(parts, axis=1).astype(bf16)
    loads[9].wait()
    wait_small(7, 8)
    first = (tokens + rms_scale(mul(head_out, w_o[...]), post_gain[...][None, :])).astype(bf16)
    moe_in = rms_scale(first, moe_gain[...][None, :]).astype(bf16)
    rows[0] = moe_in

    def row_copy(hop, src, dst):
        return pltpu.make_async_remote_copy(
            src_ref=rows.at[src],
            dst_ref=rows.at[dst],
            send_sem=send_sem.at[1],
            recv_sem=row_recv.at[dst],
            device_id=peer(hop),
            device_id_type=MESH,
        )

    def home_copy(k, hop, recv_sem):
        return pltpu.make_async_remote_copy(
            src_ref=to_home.at[k],
            dst_ref=from_home.at[k],
            send_sem=send_sem.at[2],
            recv_sem=recv_sem,
            device_id=peer(hop),
            device_id_type=MESH,
        )

    near = [1] if groups > 1 else []
    far = list(range(groups - 1, 1, -1))
    single = [m for m in range(1, size) if m & (m - 1) == 0]
    joint = [m for m in range(1, size) if m & (m - 1)]

    def spread_base(g, ms):
        for m in ms:
            row_copy(m, g * size, g * size + m).start()

    def arrive(k):
        row_copy(1, 0, k).wait_recv()

    for g in far + near:
        row_copy(g * size, 0, g * size).start()
    spread_base(0, single + joint)
    whole(s_in, load_sem.at[10]).wait()
    whole(s_down, load_sem.at[11]).wait()
    hidden = (jax.nn.silu(mul(moe_in, s_in[0])) * mul(moe_in, s_in[1])).astype(bf16)
    shared_out = mul(hidden, s_down[...])

    wait_small(9, 10)
    gate_rows = jnp.broadcast_to(dense_vec[...][None, :], (seqs, width))

    def wait_weights():
        for ref, sem in ((e_in, 12), (e_down, 13), (d_in, 6), (d_down, 7)):
            whole(ref.at[0], load_sem.at[sem]).wait()
        for ref, sem in twin:
            whole(ref.at[1], twin_sem.at[1, sem]).wait()
        whole(route_in, meta_sem.at[0]).wait()

    def weight_of(k):
        flat = route_out[me] if k == 0 else route_in[k - 1]
        return upright(flat[:, :seqs])

    def compute(start, stop):
        lo, hi = start * size, stop * size
        block = rows[lo:hi].reshape((hi - lo) * seqs, width)
        weights = jnp.concatenate([weight_of(k) for k in range(lo, hi)], axis=0)
        gate = jax.nn.sigmoid(mul_t(block, gate_rows)[:, :1])
        pairs = [(ref[c], down[c]) for ref, down in ((e_in, e_down), (d_in, d_down)) for c in range(2)]
        opened = [(mul(block, pair[0]), mul(block, pair[1])) for pair, _ in pairs]
        acts = [(jax.nn.silu(x) * y).astype(bf16) for x, y in opened]
        outs = [mul(x, down) for x, (_, down) in zip(acts, pairs)]
        routed = sum(x.astype(bf16).astype(f32) for x in outs[:2])
        part = routed * weights + (outs[2] + outs[3]) * gate
        keep[lo:hi] = part.reshape(hi - lo, seqs, width)

    def home_near():
        for m in joint + single + [0]:
            to_home[size + m] = keep[size + m].astype(bf16)
            home_copy(size + m, size, near_recv.at[m]).start()

    def gather_near(ms):
        for m in ms:
            part = keep[m]
            if near:
                home_copy(size + m, 1, near_recv.at[m]).wait_recv()
                part = part + from_home[size + m].astype(f32)
            if m > 0:
                to_home[m] = part.astype(bf16)
                home_copy(m, m, plane_recv.at[0]).start()
            else:
                keep[0] = part

    def home(g, ms):
        for m in ms:
            to_home[g * size + m] = keep[g * size + m].astype(bf16)
            home_copy(g * size + m, m, plane_recv.at[g]).start()

    def plane_sum(g):
        part = keep[g * size]
        if size > 1:
            whole(from_home.at[pl.ds(g * size + 1, size - 1)], plane_recv.at[g]).wait()
        for m in range(1, size):
            part = part + from_home[g * size + m].astype(f32)
        return part

    def send_far(g):
        to_home[g * size] = plane_sum(g).astype(bf16)
        home_copy(g * size, g * size, far_recv.at[g]).start()

    for m in single:
        arrive(m)
        for g in near:
            row_copy(size, m, size + m).start()
    for g in far:
        arrive(g * size)
        spread_base(g, joint + single)
    for m in joint:
        arrive(m)
        for g in near:
            row_copy(size, m, size + m).start()
    wait_weights()
    compute(0, 1)
    def far_turn(g):
        for m in range(1, size):
            arrive(g * size + m)
        compute(g, g + 1)
        home(g, joint + single)

    for g in far[:1]:
        far_turn(g)
    if near:
        for m in range(size):
            arrive(size + m)
        compute(1, 2)
        home_near()
    for g in far[1:]:
        far_turn(g)
    for g in far[:1]:
        send_far(g)
    gather_near(joint + single)
    for g in far[1:]:
        send_far(g)
    gather_near([0])
    total = shared_out + plane_sum(0)
    for g in far:
        home_copy(g * size, 1, far_recv.at[g]).wait_recv()
        total = total + from_home[g * size].astype(f32)
    inverse = lax.rsqrt(jnp.mean(total * total, axis=-1, keepdims=True) + eps)
    out_ref[...] = (
        first.astype(f32) + total * inverse * out_gain[...][None, :].astype(f32)
    ).astype(bf16)

    for ref, sem in twin:
        whole(ref.at[1], twin_sem.at[0, sem]).wait()
    whole(route_in, send_sem.at[0]).wait()
    whole(rows.at[pl.ds(1, count - 1)], send_sem.at[1]).wait()
    whole(to_home.at[pl.ds(1, count - 1)], send_sem.at[2]).wait()


def shards(
    tokens,
    lengths,
    cache_latent,
    cache_rope,
    attn_gain,
    w_dq,
    q_gain,
    w_q_nope,
    w_q_rope,
    w_dkv,
    kv_gain,
    w_krope,
    w_uk,
    w_uv,
    w_o,
    post_gain,
    moe_gain,
    routes,
    route_scores,
    expert_gate,
    expert_up,
    expert_down,
    shared_gate,
    shared_up,
    shared_down,
    dense_vec,
    dense_w_gate,
    dense_w_up,
    dense_w_down,
    out_gain,
):
    f32, bf16 = jnp.float32, jnp.bfloat16
    count = lax.axis_size("ep")
    groups = min(4, count)
    seqs, width = tokens.shape
    _, length, wide = cache_latent.shape
    batch = 128 // HEADS
    batches = seqs // batch
    small = [tokens, lengths, routes.T, route_scores.T, attn_gain, q_gain, kv_gain]
    small += [post_gain, moe_gain, dense_vec, out_gain]
    big = [w_dq, w_dkv, w_krope.T, w_q_nope, w_q_rope, w_uk, cache_latent, cache_rope, w_uv, w_o]
    big += [shared_gate, shared_up, shared_down, expert_gate, expert_up, dense_w_gate, dense_w_up]
    big += [expert_down, dense_w_down]
    room = [pltpu.VMEM(w.shape, w.dtype) for w in small + big[:10]]
    room[17] = pltpu.VMEM((batches, length, batch * wide), bf16)
    room[18] = pltpu.VMEM((batches, batch) + cache_rope.shape[1:], bf16)
    room += [
        pltpu.VMEM((2,) + shared_gate.shape, bf16),
        pltpu.VMEM(shared_down.shape, bf16),
        pltpu.VMEM((2, 2) + expert_gate.shape[1:], bf16),
        pltpu.VMEM((2,) + expert_down.shape[1:], bf16),
        pltpu.VMEM((2, 2) + dense_w_gate.shape, bf16),
        pltpu.VMEM((2,) + dense_w_down.shape, bf16),
    ]
    vmem = pl.BlockSpec(memory_space=pltpu.VMEM)
    dma = pltpu.SemaphoreType.DMA
    blocks = (count, seqs, width)
    tall = HEADS * batch
    experts = expert_gate.shape[0] * count
    return pl.pallas_call(
        functools.partial(layer_kernel, count, groups),
        out_shape=(pltpu.VMEM((seqs, width), bf16), pltpu.VMEM((seqs, wide), bf16)),
        in_specs=[pl.BlockSpec(memory_space=pltpu.HBM)] * (len(small) + len(big)),
        out_specs=(vmem, vmem),
        scratch_shapes=room
        + [
            pltpu.VMEM((batches, tall, wide), f32),
            pltpu.VMEM((batches, tall, batch * ROPE), f32),
            pltpu.VMEM((tall, length), f32),
            pltpu.VMEM((tall, length), bf16),
            pltpu.VMEM((batches, tall, wide), f32),
            pltpu.VMEM(blocks, bf16),
            pltpu.VMEM((experts, 1, 128), f32),
            pltpu.VMEM((count - 1, 1, 128), f32),
            pltpu.VMEM(blocks, f32),
            pltpu.VMEM(blocks, bf16),
            pltpu.VMEM(blocks, bf16),
            dma((len(small),)),
            dma((14,)),
            dma((3, batches)),
            dma((2, 4)),
            dma((1,)),
            dma((3,)),
            dma((count,)),
            dma((count // groups,)),
            dma((groups,)),
            dma((groups,)),
        ],
        compiler_params=pltpu.CompilerParams(collective_id=0, has_side_effects=True),
        name="layer",
    )(*small, *big)


def solution(mesh):
    return jax.shard_map(
        shards,
        mesh=mesh,
        in_specs=(
            P(("ep", "tp"), None),
            P(("ep", "tp")),
            P(("ep", "tp"), None, None),
            P(("ep", "tp"), None, None),
            P(),
            P(),
            P(),
            P(),
            P(),
            P(),
            P(),
            P(),
            P(),
            P(),
            P(),
            P(),
            P(),
            P(("ep", "tp"), None),
            P(("ep", "tp"), None),
            P("ep", None, "tp"),
            P("ep", None, "tp"),
            P("ep", "tp", None),
            P(),
            P(),
            P(),
            P(),
            P(None, ("ep", "tp")),
            P(None, ("ep", "tp")),
            P(("ep", "tp"), None),
            P(),
        ),
        out_specs=(P(("ep", "tp"), None), P(("ep", "tp"), None)),
        check_vma=False,
    )
```
